32 devices in a mesh: grp: 2 (over x), ep: 16 (over z, y, core).
Axes of the slice: x: 2, y: 2, z: 4, core: 2. Of those that a mesh axis runs over, the one named last changes fastest.
Arguments:
- tokens: bfloat16 [8192, 2048], P(('grp', 'ep')), parts along dimension 0, may hold values from -6 to 6
- norm_gain: float32 [2048], replicated, may hold values from 0.1 to 1.9
- route_ids: int32 [8192, 2], P(('grp', 'ep')), parts along dimension 0, may hold values from 0 to 15, as said below
- route_slots: int32 [8192, 2], P(('grp', 'ep')), parts along dimension 0, may hold values from 0 to 47, as said below
- route_weights: float32 [8192, 2], P(('grp', 'ep')), parts along dimension 0, may hold values from 0.1 to 1
- w_gate: bfloat16 [16, 2048, 512], P('ep'), may hold values from -0.125 to 0.125
- w_up: bfloat16 [16, 2048, 512], P('ep'), may hold values from -0.125 to 0.125
- w_down: bfloat16 [16, 512, 2048], P('ep'), may hold values from -0.25 to 0.25
Outputs:
- expert_mix: bfloat16 [8192, 2048], P(('grp', 'ep')), parts along dimension 0
The draws below stay inside these ranges and needn't reach their ends.
There are 2 independent parts, one for each index of `grp`. The reference program is written for one: setup_inputs(seed, part) draws one part's arguments, and reference() takes and returns one part's arrays. A program takes and returns all parts, laid end to end along the dimension named above; an argument that names none is the same for every part. Nothing has to cross between parts.
Inputs may be any that keep to these rules, and one draw needn't show every extreme that they name: `route_ids`: expert e belongs to group e // 4. Each token names 2 different experts of one group. In each aligned block of 256 tokens (the rows of one device) no expert is named more than 48 times, and some expert exactly 48 times. `route_slots`: in each aligned block of 256 tokens, the entries that name one expert hold distinct slots 0, 1, ... up to their count less one.
All inputs are finite; a program needn't handle non-finite values.
Results may differ from the reference program's by a relative error of at most 0.007.
Values may be sent and summed in bfloat16 or wider, within the bound.
No kernel may reach another device: no remote copies, remote signals or barrier semaphores. Data moves between devices by JAX's collectives and lax.ppermute only.
A program may use at most 64 MiB of HBM per device.

```python
import math
import jax
import jax.numpy as jnp
from jax import lax

D = 2048
FE = 512
TOPK = 2
TOK_DEV = 256
EXPERTS = 16
CAP = 48
TOKENS = 4096


def route_table(key):
    n_blocks = TOKENS // TOK_DEV
    per_group = EXPERTS // 4
    busy_count = CAP * per_group // 2
    rest_count = TOK_DEV - busy_count
    block_keys = jax.random.split(jax.random.fold_in(key, 7), n_blocks)

    def one_block(block_key):
        key_busy, key_first, key_second, key_perm, key_base, key_shift = jax.random.split(block_key, 6)
        busy = jax.random.randint(key_busy, (), 0, 4)
        low_first = jnp.maximum(0, rest_count - 2 * busy_count)
        high_first = jnp.minimum(busy_count, rest_count)
        count_first = jax.random.randint(key_first, (), low_first, high_first + 1)
        low_second = jnp.maximum(0, rest_count - count_first - busy_count)
        high_second = jnp.minimum(busy_count, rest_count - count_first)
        count_second = jax.random.randint(key_second, (), low_second, high_second + 1)
        others = jnp.stack([count_first, count_second, rest_count - count_first - count_second]).astype(jnp.int32)
        group_ids = jnp.arange(4, dtype=jnp.int32)
        other_idx = jnp.clip(group_ids - (group_ids > busy).astype(jnp.int32), 0, 2)
        counts = jnp.where(group_ids == busy, busy_count, others[other_idx]).astype(jnp.int32)
        ends = jnp.cumsum(counts)
        starts = ends - counts
        places = jnp.arange(TOK_DEV, dtype=jnp.int32)
        group_sorted = jnp.sum((places[:, None] >= ends[None, :3]).astype(jnp.int32), axis=1)
        rank_sorted = places - starts[group_sorted]
        perm = jax.random.permutation(key_perm, TOK_DEV)
        group_tok = jnp.zeros((TOK_DEV,), jnp.int32).at[perm].set(group_sorted)
        rank_tok = jnp.zeros((TOK_DEV,), jnp.int32).at[perm].set(rank_sorted)
        base = jax.random.randint(key_base, (4,), 0, per_group)
        shift = jax.random.randint(key_shift, (4,), 1, per_group)
        first = group_tok * per_group + (base[group_tok] + rank_tok) % per_group
        second = group_tok * per_group + (base[group_tok] + rank_tok + shift[group_tok]) % per_group
        ids = jnp.stack([first, second], axis=1).astype(jnp.int32)
        flat_ids = ids.reshape(-1)
        onehot = (flat_ids[:, None] == jnp.arange(EXPERTS, dtype=jnp.int32)[None, :]).astype(jnp.int32)
        slots = jnp.sum(jnp.cumsum(onehot, axis=0) * onehot, axis=1) - 1
        return (ids, slots.reshape(TOK_DEV, 2).astype(jnp.int32))
    ids, slots = jax.vmap(one_block)(block_keys)
    return (ids.reshape(TOKENS, 2), slots.reshape(TOKENS, 2))


def draw_route_ids(key, part):
    return route_table(key)[0]


def draw_route_slots(key, part):
    return route_table(key)[1]


def block_levels(rng, extent, shards, low, largest):
    loudness, own = 1.0, jax.random.fold_in(rng, 6)
    for dim, shards_of in shards:
        heights = jnp.exp(jax.random.uniform(jax.random.fold_in(own, dim), (shards_of,), jnp.float32, low / len(shards), largest / len(shards)))
        loudness = loudness * jnp.repeat(heights, extent[dim] // shards_of).reshape([-1 if axis == dim else 1 for axis in range(len(extent))])
    return loudness


def scatter_about(key, dims, spread, reach, cuts=(), kind=jnp.bfloat16):
    drawn = spread * jax.random.normal(key, dims, jnp.float32)
    if cuts:
        drawn = drawn * block_levels(key, dims, cuts, -0.22, 0.18)
    return jnp.clip(drawn, -reach, reach).astype(kind)


def setup_inputs(seed: int = 0, part: int = 0) -> dict:
    streams_of = jax.random.split(jax.random.key(seed), 9)
    own_keys = jax.random.split(jax.random.fold_in(streams_of[8], part), 9)
    return {
        "tokens": scatter_about(own_keys[0], (TOKENS, D), 1.0, 6.0, ((0, 16),)),
        "norm_gain": jnp.clip(1.0 + 0.18 * jax.random.normal(streams_of[1], (D,), jnp.float32), 0.1, 1.9),
        "route_ids": draw_route_ids(jax.random.fold_in(jax.random.fold_in(streams_of[8], part), 71), part),
        "route_slots": draw_route_slots(jax.random.fold_in(jax.random.fold_in(streams_of[8], part), 71), part),
        "route_weights": jnp.clip(jnp.exp(math.log(1.0) - 2.3025851 * jax.random.uniform(own_keys[4], (TOKENS, TOPK), jnp.float32) ** block_levels(own_keys[4], (TOKENS, TOPK), ((0, 16),), -0.2, 0.2)), 0.1, 1.0),
        "w_gate": scatter_about(streams_of[5], (EXPERTS, D, FE), D ** -0.5, 0.125, ((0, 16),)),
        "w_up": scatter_about(streams_of[6], (EXPERTS, D, FE), D ** -0.5, 0.125, ((0, 16),)),
        "w_down": scatter_about(streams_of[7], (EXPERTS, FE, D), FE ** -0.5, 0.25, ((0, 16),)),
    }


def reference(tokens, norm_gain, route_ids, route_slots, route_weights, w_gate, w_up, w_down):
    tok_f32 = tokens.astype(jnp.float32)
    scale = lax.rsqrt(lax.optimization_barrier(jnp.mean(tok_f32 * tok_f32, axis=-1, keepdims=True)) + 1e-06)
    normed = (tok_f32 * scale * norm_gain.astype(jnp.float32)).astype(jnp.bfloat16)
    n_blocks = TOKENS // TOK_DEV
    block_of = (jnp.arange(TOKENS, dtype=jnp.int32) // TOK_DEV).astype(jnp.int32)
    place_idx = (route_ids * (n_blocks * CAP) + block_of[:, None] * CAP + route_slots).astype(jnp.int32)
    buffer = jnp.zeros((EXPERTS * n_blocks * CAP, D), jnp.bfloat16)
    buffer = buffer.at[place_idx.reshape(-1)].set(jnp.repeat(normed, TOPK, axis=0))
    buffer = buffer.reshape(EXPERTS, n_blocks * CAP, D)

    def expert_apply(args):
        rows_in, gate_w, up_w, down_w = args
        gate_act = jnp.dot(rows_in, gate_w, preferred_element_type=jnp.float32)
        up_act = jnp.dot(rows_in, up_w, preferred_element_type=jnp.float32)
        hidden = (jax.nn.silu(gate_act) * up_act).astype(jnp.bfloat16)
        return jnp.dot(hidden, down_w, preferred_element_type=jnp.float32).astype(jnp.bfloat16)
    results = lax.map(expert_apply, (buffer, w_gate, w_up, w_down))
    flat_rows = results.reshape(EXPERTS * n_blocks * CAP, D)
    picked = flat_rows[place_idx].astype(jnp.float32)
    mixed = lax.optimization_barrier(jnp.sum(route_weights[:, :, None] * picked, axis=1))
    return mixed.astype(jnp.bfloat16)
```

```python
import jax
import jax.numpy as jnp
from jax import lax
from jax.sharding import PartitionSpec as P

GROUPS = 4
LANES = 128
BF = jnp.bfloat16
F32 = jnp.float32


def split3(w):
    hi = w.astype(BF).astype(F32)
    mid = (w - hi).astype(BF).astype(F32)
    lo = w - hi - mid
    return [hi, mid, lo]


def shards(tokens, norm_gain, route_ids, route_slots, route_weights, w_gate, w_up, w_down):
    tok_rows, feat = tokens.shape
    n_devices = lax.axis_size("ep")
    local_count = w_gate.shape[0]
    experts_all = n_devices * local_count
    top = route_ids.shape[1]
    capacity = 3 * top * tok_rows // (2 * experts_all)
    span = n_devices // GROUPS
    per_group = experts_all // GROUPS
    rows = capacity * per_group // top
    me = lax.axis_index("ep")
    my_group = me // span

    def group_perm(s):
        return [(d, ((d // span) ^ s) * span + d % span) for d in range(n_devices)]

    def inner_perm(b):
        return [(d, d ^ b) for d in range(n_devices)]

    bits = []
    b = span // 2
    while b:
        bits.append(b)
        b //= 2

    tok_f32 = tokens.astype(F32)
    scale = lax.rsqrt(jnp.mean(tok_f32 * tok_f32, axis=-1, keepdims=True) + 1e-06)
    normed = (tok_f32 * scale * norm_gain).astype(BF)

    cols = []
    for k in range(top):
        cols += [route_ids[:, k] % per_group + 1, route_slots[:, k]]
    cols = [c.astype(F32) for c in cols]
    for k in range(top):
        cols += split3(route_weights[:, k])
    meta = jnp.stack(cols, axis=1).astype(BF)
    meta = jnp.pad(meta, ((0, 0), (0, LANES - meta.shape[1])))

    grp = route_ids[:, 0] // per_group
    same = grp[:, None] == grp[None, :]
    earlier = lax.broadcasted_iota(jnp.int32, same.shape, 0) > lax.broadcasted_iota(jnp.int32, same.shape, 1)
    rank = jnp.sum((same & earlier).astype(jnp.int32), axis=1)
    place = (grp ^ my_group) * rows + rank
    pick = (lax.broadcasted_iota(jnp.int32, (GROUPS * rows, tok_rows), 0) == place[None, :]).astype(BF)

    payload = jnp.concatenate([normed, meta], axis=1)
    packed = jnp.dot(pick, payload, preferred_element_type=F32).astype(BF)

    my_first = (me % span) * local_count

    def expert(block):
        blocks = span
        wide = block.shape[0]
        info = block[:, feat:].astype(F32)
        out_rows = blocks * capacity
        block_of_row = lax.broadcasted_iota(jnp.int32, (out_rows, wide), 1) // rows
        slot_row = lax.broadcasted_iota(jnp.int32, (out_rows, wide), 0)
        total = None
        for x in range(local_count):
            mine = (my_first + x + 1).astype(F32)
            at = jnp.full((wide,), -1, jnp.int32)
            weight = jnp.zeros((wide,), F32)
            for k in range(top):
                hit = info[:, 2 * k] == mine
                at = jnp.where(hit, info[:, 2 * k + 1].astype(jnp.int32), at)
                base = 2 * top + 3 * k
                w = info[:, base] + info[:, base + 1] + info[:, base + 2]
                weight = weight + jnp.where(hit, w, 0.0)
            sel = ((slot_row == block_of_row * capacity + at[None, :]) & (at >= 0)[None, :]).astype(BF)
            rows_in = jnp.dot(sel, block[:, :feat], preferred_element_type=F32).astype(BF)
            gate = jnp.dot(rows_in, w_gate[x], preferred_element_type=F32)
            up = jnp.dot(rows_in, w_up[x], preferred_element_type=F32)
            hidden = (jax.nn.silu(gate) * up).astype(BF)
            res = jnp.dot(hidden, w_down[x], preferred_element_type=F32).astype(BF)
            back = lax.dot_general(sel, res, (((0,), (0,)), ((), ())), preferred_element_type=F32)
            part = back * weight[:, None]
            total = part if total is None else total + part
        return total.astype(BF)

    def chunk(s, after):
        block = packed[s * rows:(s + 1) * rows]
        if after is not None:
            block, _ = lax.optimization_barrier((block, after))
        if s:
            block = lax.ppermute(block, "ep", group_perm(s))
        for b in bits:
            block = jnp.concatenate([block, lax.ppermute(block, "ep", inner_perm(b))], axis=0)
        part = expert(block)
        for b in reversed(bits):
            half = part.shape[0] // 2
            got = lax.ppermute(part[half:], "ep", inner_perm(b))
            part = (part[:half].astype(F32) + got.astype(F32)).astype(BF)
        if s:
            part = lax.ppermute(part, "ep", group_perm(s))
        return part

    order = [0, 1, 2, 3]
    done, last = {}, None
    for s in order:
        last = done[s] = chunk(s, last if span > GROUPS else None)
    home = jnp.concatenate([done[s] for s in range(GROUPS)], axis=0)
    mixed = lax.dot_general(pick, home, (((0,), (0,)), ((), ())), preferred_element_type=F32)
    return mixed.astype(BF)


def solution(mesh):
    placed = (
        P(("grp", "ep"), None),
        P(),
        P(("grp", "ep"), None),
        P(("grp", "ep"), None),
        P(("grp", "ep"), None),
        P("ep", None, None),
        P("ep", None, None),
        P("ep", None, None),
    )
    return jax.shard_map(
        shards, mesh=mesh, in_specs=placed, out_specs=P(("grp", "ep"), None), check_vma=False
    )
```

```python
import functools

import jax
import jax.numpy as jnp
from jax import lax
from jax.experimental import pallas as pl
from jax.experimental.pallas import tpu as pltpu
from jax.sharding import PartitionSpec as P

GROUPS = 4
LANES = 128
BF = jnp.bfloat16
F32 = jnp.float32


def split3(w):
    hi = w.astype(BF).astype(F32)
    mid = (w - hi).astype(BF).astype(F32)
    lo = w - hi - mid
    return [hi, mid, lo]


def expert_kernel(top, capacity, rows, first_ref, *refs):
    blocks, (gate_ref, up_ref, down_ref, low_ref, high_ref) = refs[:-5], refs[-5:]
    count = len(blocks)
    feat = low_ref.shape[1]
    info = jnp.concatenate([r[:, feat:] for r in blocks], axis=0).astype(F32)
    wide = count * rows
    slots = count * capacity
    lane = lax.broadcasted_iota(jnp.int32, (wide, slots), 1)
    base_slot = jnp.concatenate([jnp.full((rows, 1), i * capacity, jnp.int32) for i in range(count)], axis=0)
    for x in range(gate_ref.shape[0]):
        mine = (first_ref[0] + x + 1).astype(F32)
        at = jnp.full((wide, 1), -float(slots), F32)
        weight = jnp.zeros((wide, 1), F32)
        for k in range(top):
            hit = info[:, 2 * k:2 * k + 1] == mine
            at = jnp.where(hit, info[:, 2 * k + 1:2 * k + 2], at)
            c = 2 * top + 3 * k
            weight = weight + jnp.where(hit, info[:, c:c + 1] + info[:, c + 1:c + 2] + info[:, c + 2:c + 3], 0.0)
        sel = jnp.where(lane == base_slot + at.astype(jnp.int32), 1.0, 0.0).astype(BF)
        sel_t = jnp.transpose(sel)
        rows_in = None
        for i in range(count):
            piece = jnp.dot(sel_t[i * capacity:(i + 1) * capacity, i * rows:(i + 1) * rows], blocks[i][:, :feat], preferred_element_type=F32).astype(BF)
            rows_in = [piece] if rows_in is None else rows_in + [piece]
        rows_in = jnp.concatenate(rows_in, axis=0)
        g = jnp.dot(rows_in, gate_ref[x], preferred_element_type=F32)
        u = jnp.dot(rows_in, up_ref[x], preferred_element_type=F32)
        hidden = (g / (1.0 + jnp.exp(-g)) * u).astype(BF)
        res = jnp.dot(hidden, down_ref[x], preferred_element_type=F32).astype(BF)
        for i in range(count):
            part = jnp.dot(
                sel[i * rows:(i + 1) * rows, i * capacity:(i + 1) * capacity],
                res[i * capacity:(i + 1) * capacity],
                preferred_element_type=F32,
            ) * weight[i * rows:(i + 1) * rows]
            ref, j = (low_ref, i) if i < count // 2 else (high_ref, i - count // 2)
            spot = pl.ds(j * rows, rows)
            if x:
                part = part + ref[spot, :].astype(F32)
            ref[spot, :] = part.astype(BF)


def shards(tokens, norm_gain, route_ids, route_slots, route_weights, w_gate, w_up, w_down):
    tok_rows, feat = tokens.shape
    n_devices = lax.axis_size("ep")
    local_count = w_gate.shape[0]
    experts_all = n_devices * local_count
    top = route_ids.shape[1]
    capacity = 3 * top * tok_rows // (2 * experts_all)
    span = n_devices // GROUPS
    per_group = experts_all // GROUPS
    rows = capacity * per_group // top
    me = lax.axis_index("ep")
    my_group = me // span

    def group_perm(s):
        return [(d, ((d // span) ^ s) * span + d % span) for d in range(n_devices)]

    def inner_perm(b):
        return [(d, d ^ b) for d in range(n_devices)]

    bits = []
    b = span // 2
    while b:
        bits.append(b)
        b //= 2

    tok_f32 = tokens.astype(F32)
    scale = lax.rsqrt(jnp.mean(tok_f32 * tok_f32, axis=-1, keepdims=True) + 1e-06)
    normed = (tok_f32 * scale * norm_gain).astype(BF)

    cols = []
    for k in range(top):
        cols += [route_ids[:, k] % per_group + 1, route_slots[:, k]]
    cols = [c.astype(F32) for c in cols]
    for k in range(top):
        cols += split3(route_weights[:, k])
    meta = jnp.stack(cols, axis=1).astype(BF)
    meta = jnp.pad(meta, ((0, 0), (0, LANES - meta.shape[1])))

    grp = route_ids[:, 0] // per_group
    same = grp[:, None] == grp[None, :]
    earlier = lax.broadcasted_iota(jnp.int32, same.shape, 0) > lax.broadcasted_iota(jnp.int32, same.shape, 1)
    rank = jnp.sum((same & earlier).astype(jnp.int32), axis=1)
    place = (grp ^ my_group) * rows + rank
    pick = (lax.broadcasted_iota(jnp.int32, (GROUPS * rows, tok_rows), 0) == place[None, :]).astype(BF)

    payload = jnp.concatenate([normed, meta], axis=1)
    packed = jnp.dot(pick, payload, preferred_element_type=F32).astype(BF)

    my_first = ((me % span) * local_count).astype(jnp.int32).reshape(1)

    def expert(blocks):
        shape = functools.partial(jax.ShapeDtypeStruct, dtype=BF)
        half = span * rows // 2
        work = span * capacity * local_count
        sizes = span * rows * (8 * feat + 4 * LANES) + 3 * 2 * w_gate.size + work * 20 * feat
        return pl.pallas_call(
            functools.partial(expert_kernel, top, capacity, rows),
            out_shape=[shape((half, feat)), shape((half, feat))],
            in_specs=[pl.BlockSpec(memory_space=pltpu.SMEM)] + [pl.BlockSpec(memory_space=pltpu.VMEM)] * (span + 3),
            out_specs=[pl.BlockSpec(memory_space=pltpu.VMEM)] * 2,
            compiler_params=pltpu.CompilerParams(vmem_limit_bytes=min(sizes + (8 << 20), 60 << 20)),
            cost_estimate=pl.CostEstimate(
                flops=work * feat * w_gate.shape[2] * 6, bytes_accessed=6 * w_gate.size, transcendentals=0
            ),
        )(my_first, *blocks, w_gate, w_up, w_down)

    arrived = {0: packed[:rows]}
    for s in (1, 3, 2):
        arrived[s] = lax.ppermute(packed[s * rows:(s + 1) * rows], "ep", group_perm(s))

    done, parts, last = {}, [], None
    for i, s in enumerate((0, 1, 3, 2)):
        block = arrived[s]
        gate = last if span > GROUPS else (parts[i - 2] if i >= 2 else None)
        if gate is not None:
            block, _ = lax.optimization_barrier((block, gate))
        blocks = [block]
        for b in bits:
            blocks = blocks + [lax.ppermute(x, "ep", inner_perm(b)) for x in blocks]
        low, high = expert(blocks)
        parts.append(high)
        for b in reversed(bits):
            got = lax.ppermute(high, "ep", inner_perm(b))
            n = low.shape[0] // 2 if b != bits[0] else low.shape[0]
            if b != bits[0]:
                high = (low[n:].astype(F32) + got[n:].astype(F32)).astype(BF)
            low = (low[:n].astype(F32) + got[:n].astype(F32)).astype(BF)
        if s:
            low = lax.ppermute(low, "ep", group_perm(s))
        last = done[s] = low
    home = jnp.concatenate([done[s] for s in range(GROUPS)], axis=0)
    mixed = lax.dot_general(pick, home, (((0,), (0,)), ((), ())), preferred_element_type=F32)
    return mixed.astype(BF)


def solution(mesh):
    placed = (
        P(("grp", "ep"), None),
        P(),
        P(("grp", "ep"), None),
        P(("grp", "ep"), None),
        P(("grp", "ep"), None),
        P("ep", None, None),
        P("ep", None, None),
        P("ep", None, None),
    )
    return jax.shard_map(
        shards, mesh=mesh, in_specs=placed, out_specs=P(("grp", "ep"), None), check_vma=False
    )
```

```python
import functools

import jax
import jax.numpy as jnp
from jax import lax
from jax.experimental import pallas as pl
from jax.experimental.pallas import tpu as pltpu
from jax.sharding import PartitionSpec as P


GROUPS = 4
LANES = 128
BF = jnp.bfloat16
F32 = jnp.float32


def split3(w):
    hi = w.astype(BF).astype(F32)
    mid = (w - hi).astype(BF).astype(F32)
    lo = w - hi - mid
    return [hi, mid, lo]


def expert_kernel(top, capacity, rows, first_ref, *refs):
    blocks, (gate_ref, up_ref, down_ref, low_ref, high_ref) = refs[:-5], refs[-5:]
    count = len(blocks)
    feat = low_ref.shape[1]
    info = jnp.concatenate([r[:, feat:] for r in blocks], axis=0).astype(F32)
    wide = count * rows
    slots = count * capacity
    lane = lax.broadcasted_iota(jnp.int32, (wide, slots), 1)
    base_slot = jnp.concatenate([jnp.full((rows, 1), i * capacity, jnp.int32) for i in range(count)], axis=0)
    for x in range(gate_ref.shape[0]):
        mine = (first_ref[0] + x + 1).astype(F32)
        at = jnp.full((wide, 1), -float(slots), F32)
        weight = jnp.zeros((wide, 1), F32)
        for k in range(top):
            hit = info[:, 2 * k:2 * k + 1] == mine
            at = jnp.where(hit, info[:, 2 * k + 1:2 * k + 2], at)
            c = 2 * top + 3 * k
            weight = weight + jnp.where(hit, info[:, c:c + 1] + info[:, c + 1:c + 2] + info[:, c + 2:c + 3], 0.0)
        sel = jnp.where(lane == base_slot + at.astype(jnp.int32), 1.0, 0.0).astype(BF)
        sel_t = jnp.transpose(sel)
        rows_in = None
        for i in range(count):
            piece = jnp.dot(sel_t[i * capacity:(i + 1) * capacity, i * rows:(i + 1) * rows], blocks[i][:, :feat], preferred_element_type=F32).astype(BF)
            rows_in = [piece] if rows_in is None else rows_in + [piece]
        rows_in = jnp.concatenate(rows_in, axis=0)
        g = jnp.dot(rows_in, gate_ref[x], preferred_element_type=F32)
        u = jnp.dot(rows_in, up_ref[x], preferred_element_type=F32)
        hidden = (g / (1.0 + jnp.exp(-g)) * u).astype(BF)
        res = jnp.dot(hidden, down_ref[x], preferred_element_type=F32).astype(BF)
        for i in range(count):
            part = jnp.dot(
                sel[i * rows:(i + 1) * rows, i * capacity:(i + 1) * capacity],
                res[i * capacity:(i + 1) * capacity],
                preferred_element_type=F32,
            ) * weight[i * rows:(i + 1) * rows]
            ref, j = (low_ref, i) if i < count // 2 else (high_ref, i - count // 2)
            spot = pl.ds(j * rows, rows)
            if x:
                part = part + ref[spot, :].astype(F32)
            ref[spot, :] = part.astype(BF)


def send(x, perm):
    return lax.ppermute(x, "ep", perm)


def layer(tokens, norm_gain, route_ids, route_slots, route_weights, w_gate, w_up, w_down):
    tok_rows, feat = tokens.shape
    n_devices = lax.axis_size("ep")
    local_count = w_gate.shape[0]
    experts_all = n_devices * local_count
    top = route_ids.shape[1]
    capacity = 3 * top * tok_rows // (2 * experts_all)
    span = n_devices // GROUPS
    per_group = experts_all // GROUPS
    rows = capacity * per_group // top
    me = lax.axis_index("ep")
    my_group = me // span

    def group_perm(s):
        return [(d, ((d // span) ^ s) * span + d % span) for d in range(n_devices)]

    def inner_perm(b):
        return [(d, d ^ b) for d in range(n_devices)]

    bits = []
    b = span // 2
    while b:
        bits.append(b)
        b //= 2

    tok_f32 = tokens.astype(F32)
    scale = lax.rsqrt(jnp.mean(tok_f32 * tok_f32, axis=-1, keepdims=True) + 1e-06)
    normed = (tok_f32 * scale * norm_gain).astype(BF)

    cols = []
    for k in range(top):
        cols += [route_ids[:, k] % per_group + 1, route_slots[:, k]]
    cols = [c.astype(F32) for c in cols]
    for k in range(top):
        cols += split3(route_weights[:, k])
    meta = jnp.stack(cols, axis=1).astype(BF)
    meta = jnp.pad(meta, ((0, 0), (0, LANES - meta.shape[1])))

    grp = route_ids[:, 0] // per_group
    same = grp[:, None] == grp[None, :]
    earlier = lax.broadcasted_iota(jnp.int32, same.shape, 0) > lax.broadcasted_iota(jnp.int32, same.shape, 1)
    rank = jnp.sum((same & earlier).astype(jnp.int32), axis=1)
    place = (grp ^ my_group) * rows + rank
    pick = (lax.broadcasted_iota(jnp.int32, (GROUPS * rows, tok_rows), 0) == place[None, :]).astype(BF)

    payload = jnp.concatenate([normed, meta], axis=1)
    packed = jnp.dot(pick, payload, preferred_element_type=F32).astype(BF)

    my_first = ((me % span) * local_count).astype(jnp.int32).reshape(1)

    def expert(blocks):
        shape = functools.partial(jax.ShapeDtypeStruct, dtype=BF)
        half = span * rows // 2
        work = span * capacity * local_count
        sizes = span * rows * (8 * feat + 4 * LANES) + 3 * 2 * w_gate.size + work * 20 * feat
        return pl.pallas_call(
            functools.partial(expert_kernel, top, capacity, rows),
            out_shape=[shape((half, feat)), shape((half, feat))],
            in_specs=[pl.BlockSpec(memory_space=pltpu.SMEM)] + [pl.BlockSpec(memory_space=pltpu.VMEM)] * (span + 3),
            out_specs=[pl.BlockSpec(memory_space=pltpu.VMEM)] * 2,
            compiler_params=pltpu.CompilerParams(vmem_limit_bytes=min(sizes + (8 << 20), 60 << 20)),
            cost_estimate=pl.CostEstimate(
                flops=work * feat * w_gate.shape[2] * 6, bytes_accessed=6 * w_gate.size, transcendentals=0
            ),
        )(my_first, *blocks, w_gate, w_up, w_down)

    arrived = {0: packed[:rows]}
    for s in (1, 3, 2):
        arrived[s] = send(packed[s * rows:(s + 1) * rows], group_perm(s))

    done, last = {}, None
    for s in (0, 1, 3, 2):
        block = arrived[s]
        if last is not None and span > GROUPS:
            block, _ = lax.optimization_barrier((block, last))
        blocks = [block]
        for b in bits:
            blocks = blocks + [send(x, inner_perm(b)) for x in blocks]
        low, high = expert(blocks)
        for b in reversed(bits):
            got = send(high, inner_perm(b))
            n = low.shape[0] // 2 if b != bits[0] else low.shape[0]
            if b != bits[0]:
                high = (low[n:].astype(F32) + got[n:].astype(F32)).astype(BF)
            low = (low[:n].astype(F32) + got[:n].astype(F32)).astype(BF)
        if s:
            low = send(low, group_perm(s))
        last = done[s] = low
    home = jnp.concatenate([done[s] for s in range(GROUPS)], axis=0)
    mixed = lax.dot_general(pick, home, (((0,), (0,)), ((), ())), preferred_element_type=F32)
    return mixed.astype(BF)


def solution(mesh):
    placed = (
        P(("grp", "ep"), None),
        P(),
        P(("grp", "ep"), None),
        P(("grp", "ep"), None),
        P(("grp", "ep"), None),
        P("ep", None, None),
        P("ep", None, None),
        P("ep", None, None),
    )
    return jax.shard_map(layer, mesh=mesh, in_specs=placed, out_specs=P(("grp", "ep"), None), check_vma=False)
```
